32 devices in a mesh: sp: 8 (over z, y), tp: 4 (over x, core).
Axes of the slice: x: 2, y: 2, z: 4, core: 2. Of those that a mesh axis runs over, the one named last changes fastest.
Arguments:
- tokens: bfloat16 [2560, 2048], P('sp', 'tp'), may hold values from -6 to 6
- pre_gain: float32 [2, 2048], replicated, may hold values from 0.1 to 1.9
- w_value: bfloat16 [2, 2048, 2048], P(None, 'sp', 'tp'), may hold values from -0.125 to 0.125
- w_gate: bfloat16 [2, 2048, 2048], P(None, 'sp', 'tp'), may hold values from -0.125 to 0.125
- taps: float32 [2, 31, 2048], P(None, None, 'tp'), may hold values from -5 to 5
- norm_gain: float32 [2, 2048], P(None, 'tp'), may hold values from 0.1 to 1.9
- norm_shift: float32 [2, 2048], P(None, 'tp'), may hold values from -3 to 3
- w_out: bfloat16 [2, 2048, 2048], P(None, 'tp', 'sp'), may hold values from -2 to 2
- post_gain: float32 [2, 2048], P(None, 'tp'), may hold values from 0.1 to 1.9
Outputs:
- stream: bfloat16 [2560, 2048], P('sp', 'tp')
The draws below stay inside these ranges and needn't reach their ends.
All inputs are finite; a program needn't handle non-finite values.
Results may differ from the reference program's by a relative error of at most 0.015.
Values may be sent and summed in bfloat16 or wider, within the bound.
No kernel may reach another device: no remote copies, remote signals or barrier semaphores. Data moves between devices by JAX's collectives and lax.ppermute only.
A program may use at most 64 MiB of HBM per device.

```python
import jax
import jax.numpy as jnp
from jax import lax

D = 2048
CONV_WIDTH = 31
LAYERS = 2
TOKENS = 2560
N_TP = 4


def draw_taps(key, part):
    first, second, third = jax.random.split(jax.random.fold_in(key, 7), 3)
    base = jax.random.truncated_normal(first, -4.0, 4.0, (LAYERS, CONV_WIDTH, D), jnp.float32) * CONV_WIDTH ** (-0.5)
    channel = jnp.exp(jax.random.uniform(second, (LAYERS, 1, D), jnp.float32, -0.7, 0.7))
    levels = jnp.array([0.4, 0.8, 1.6, 3.2], jnp.float32)
    order = jnp.stack([jax.random.permutation(jax.random.fold_in(third, layer), 4) for layer in range(LAYERS)])
    groups = jnp.repeat(levels[order], D // 4, axis=1)
    return base * channel * groups[:, None, :]


def draw_w_out(key, part):
    first, second = jax.random.split(jax.random.fold_in(key, 11), 2)
    base = jax.random.truncated_normal(first, -4.0, 4.0, (LAYERS, D, D), jnp.float32) * D ** (-0.5)
    levels = jnp.array([0.4, 0.8, 1.6, 3.2], jnp.float32)
    order = jnp.stack([jax.random.permutation(jax.random.fold_in(second, layer), 4) for layer in range(LAYERS)])
    groups = jnp.repeat(levels[order], D // 4, axis=1)
    return (base * groups[:, None, :]).astype(jnp.bfloat16)


def shard_levels(own_key, shape, shards, low, largest):
    loudness = 1.0
    for position, parts in shards:
        draws = jax.random.uniform(jax.random.fold_in(jax.random.fold_in(own_key, 6), position), (parts,), jnp.float32, low / len(shards), largest / len(shards))
        loudness = loudness * jnp.repeat(jnp.exp(draws), shape[position] // parts).reshape((-1,) + (1,) * (len(shape) - 1 - position))
    return loudness


def noise(rng, shape, width, most, pieces=(), dtype=jnp.bfloat16):
    values = jax.random.normal(rng, shape, jnp.float32) * width
    if len(pieces) > 0:
        values = shard_levels(rng, shape, pieces, -0.22, 0.18) * values
    return jnp.clip(values, min=-most, max=most).astype(dtype)


def setup_inputs(seed: int = 0) -> dict:
    keys = jax.random.split(jax.random.key(seed), 10)
    tokens = noise(keys[0], (TOKENS, D), 1.0, 6.0, ((0, 8), (1, 4)))
    pre_gain = jnp.clip(1.0 + 0.18 * jax.random.normal(keys[1], (LAYERS, D), jnp.float32), 0.1, 1.9)
    w_value = noise(keys[2], (LAYERS, D, D), D ** -0.5, 0.125, ((1, 8), (2, 4)))
    w_gate = noise(keys[3], (LAYERS, D, D), D ** -0.5, 0.125, ((1, 8), (2, 4)))
    taps = draw_taps(jax.random.fold_in(keys[9], 71), 0)
    norm_gain = jnp.clip(1.0 + 0.18 * jax.random.normal(keys[5], (LAYERS, D), jnp.float32), 0.1, 1.9)
    norm_shift = noise(keys[6], (LAYERS, D), 0.5, 3.0, ((1, 4),), jnp.float32)
    w_out = draw_w_out(jax.random.fold_in(keys[9], 71), 0)
    post_gain = jnp.clip(1.0 + 0.18 * jax.random.normal(keys[8], (LAYERS, D), jnp.float32), 0.1, 1.9)
    return dict(tokens=tokens, pre_gain=pre_gain, w_value=w_value, w_gate=w_gate, taps=taps, norm_gain=norm_gain, norm_shift=norm_shift, w_out=w_out, post_gain=post_gain)


EPSILON = 1e-06
LN_EPSILON = 1e-05

def reference(tokens, pre_gain, w_value, w_gate, taps, norm_gain, norm_shift, w_out, post_gain):
    stream = tokens
    block = D // N_TP
    for layer in range(LAYERS):
        stream_f = stream.astype(jnp.float32)
        normed = (stream_f * lax.rsqrt(lax.optimization_barrier(jnp.mean(stream_f * stream_f, -1, keepdims=True)) + EPSILON) * pre_gain[layer]).astype(jnp.bfloat16)
        value_proj = jnp.dot(normed, w_value[layer], preferred_element_type=jnp.float32)
        gate_proj = jnp.dot(normed, w_gate[layer], preferred_element_type=jnp.float32)
        glu_act = (value_proj * jax.nn.sigmoid(gate_proj)).astype(jnp.bfloat16)
        padded = jnp.pad(glu_act.astype(jnp.float32), ((CONV_WIDTH - 1, 0), (0, 0)))
        conv_out = jnp.zeros((TOKENS, D), jnp.float32)
        for offset in range(CONV_WIDTH):
            conv_out = conv_out + taps[layer, offset] * padded[offset:offset + TOKENS]
        center = lax.optimization_barrier(jnp.sum(conv_out, -1, keepdims=True)) / D
        spread = jnp.maximum(lax.optimization_barrier(jnp.sum(conv_out * conv_out, -1, keepdims=True)) / D - center * center, 0.0)
        activated = jax.nn.silu((conv_out - center) * lax.rsqrt(spread + LN_EPSILON) * norm_gain[layer] + norm_shift[layer]).astype(jnp.bfloat16)
        summed = jnp.zeros((TOKENS, D), jnp.float32)
        for start in range(0, D, block):
            partial_sum = jnp.dot(activated[:, start:start + block], w_out[layer, start:start + block, :], preferred_element_type=jnp.float32).astype(jnp.bfloat16)
            partial_sum = lax.optimization_barrier(partial_sum)
            summed = summed + partial_sum.astype(jnp.float32)
        projected = summed.astype(jnp.bfloat16).astype(jnp.float32)
        scale = lax.rsqrt(lax.optimization_barrier(jnp.mean(projected * projected, -1, keepdims=True)) + EPSILON)
        stream = (stream_f + projected * scale * post_gain[layer]).astype(jnp.bfloat16)
    return stream
```

```python
import jax
import jax.numpy as jnp
from jax import lax
from jax.sharding import Mesh, PartitionSpec as P

EPSILON = 1e-06
LN_EPSILON = 1e-05


GROUP = ("l", "x", "c")


def swapped(block, axes):
    size = 2 ** len(axes)
    return lax.ppermute(block, axes, [(i, size - 1 - i) for i in range(size)])


def ordered(index, own, other, axis):
    return jnp.where(
        index == 0, jnp.concatenate([own, other], axis), jnp.concatenate([other, own], axis)
    )


def part(array, index, axis):
    size = array.shape[axis] // 2
    return lax.dynamic_slice_in_dim(array, index * size, size, axis)


def paired(array, cut_axis, join_axis):
    l = lax.axis_index("l")
    other = swapped(part(array, 1 - l, cut_axis), ("l",))
    return ordered(l, part(array, l, cut_axis), other, join_axis)


def all_rows(block):
    l, x, c = (lax.axis_index(a) for a in GROUP)
    from_x = swapped(block, ("x",))
    from_l = swapped(block, ("l",))
    from_lx = swapped(block, ("l", "x"))
    mine = [block, from_x, from_l, from_lx]
    theirs = [swapped(b, ("c",)) for b in mine]
    cells = []
    for m, t in zip(mine, theirs):
        cells.append((jnp.where(c == 0, m, t), jnp.where(c == 0, t, m)))
    (a0, a1), (b0, b1), (p0, p1), (q0, q1) = cells
    near = jnp.where(x == 0, jnp.concatenate([a0, a1, b0, b1], 1), jnp.concatenate([b0, b1, a0, a1], 1))
    far = jnp.where(x == 0, jnp.concatenate([p0, p1, q0, q1], 1), jnp.concatenate([q0, q1, p0, p1], 1))
    return ordered(l, near, far, 0)


def scattered_sum(activated, out_mat):
    l, x, c = (lax.axis_index(a) for a in GROUP)
    cols = out_mat.shape[1] // 4
    rows = activated.shape[0] // 2

    def terms(x_at, c_at):
        mat = lax.dynamic_slice_in_dim(out_mat, (x_at * 2 + c_at) * cols, cols, 1)
        return jnp.dot(activated, mat, preferred_element_type=jnp.float32).astype(jnp.bfloat16)

    to_far, to_near = terms(1 - x, 1 - c), terms(x, 1 - c)
    far = terms(1 - x, c).astype(jnp.float32) + swapped(to_far, ("c",)).astype(jnp.float32)
    far = far.astype(jnp.bfloat16)
    near = terms(x, c).astype(jnp.float32) + swapped(to_near, ("c",)).astype(jnp.float32)
    near = near.astype(jnp.bfloat16)
    from_lx = swapped(part(far, 1 - l, 0), ("l", "x"))
    from_x = swapped(part(far, l, 0), ("x",))
    from_l = swapped(part(near, 1 - l, 0), ("l",))
    own = part(near, l, 0)
    total = own.astype(jnp.float32) + from_x.astype(jnp.float32)
    total = total + from_l.astype(jnp.float32) + from_lx.astype(jnp.float32)
    return total.astype(jnp.bfloat16)


def local(tokens, pre_gain, w_value, w_gate, taps, norm_gain, norm_shift, w_out, post_gain):
    l, x, c = (lax.axis_index(a) for a in GROUP)
    layers, width = taps.shape[:2]
    model = pre_gain.shape[1]
    n_h = lax.axis_size("h")
    in_mats, out_mats = [], []
    for layer in range(layers):
        half = jnp.concatenate([paired(w_value[layer], 1, 0), paired(w_gate[layer], 1, 0)], 1)
        in_mats.append(lax.all_gather(half, "h", axis=0, tiled=True))
        out_mats.append(lax.all_gather(paired(w_out[layer], 0, 1), "h", axis=1, tiled=True))
    full_post = lax.all_gather(post_gain, ("x", "c"), axis=1, tiled=True)
    whole = all_rows(tokens)
    rows = whole.shape[0]
    for layer in range(layers):
        whole_f = whole.astype(jnp.float32)
        normed = (
            whole_f
            * lax.rsqrt(jnp.mean(whole_f * whole_f, -1, keepdims=True) + EPSILON)
            * pre_gain[layer]
        ).astype(jnp.bfloat16)
        proj = jnp.dot(normed, in_mats[layer], preferred_element_type=jnp.float32)
        value_proj, gate_proj = jnp.split(proj, 2, 1)
        glu_act = (value_proj * jax.nn.sigmoid(gate_proj)).astype(jnp.bfloat16)
        fringe = lax.ppermute(
            glu_act[rows - (width - 1) :], "h", [(i, i + 1) for i in range(n_h - 1)]
        )
        padded = jnp.concatenate([fringe, glu_act], 0).astype(jnp.float32)
        tap = part(taps[layer], l, 1)
        conv_out = jnp.zeros(glu_act.shape, jnp.float32)
        for offset in range(width):
            conv_out = conv_out + tap[offset] * padded[offset : offset + rows]
        row_sum, row_square = lax.psum(
            (jnp.sum(conv_out, -1, keepdims=True), jnp.sum(conv_out * conv_out, -1, keepdims=True)),
            GROUP,
        )
        center = row_sum / model
        spread = jnp.maximum(row_square / model - center * center, 0.0)
        activated = jax.nn.silu(
            (conv_out - center) * lax.rsqrt(spread + LN_EPSILON) * part(norm_gain[layer], l, 0)
            + part(norm_shift[layer], l, 0)
        ).astype(jnp.bfloat16)
        projected = scattered_sum(activated, out_mats[layer])
        if layer < layers - 1:
            added = all_rows(projected).astype(jnp.float32)
            scale = lax.rsqrt(jnp.mean(added * added, -1, keepdims=True) + EPSILON)
            whole = (whole_f + added * scale * full_post[layer]).astype(jnp.bfloat16)
        else:
            own = part(whole, l, 0)
            cols = tokens.shape[1]
            own = lax.dynamic_slice_in_dim(own, (x * 2 + c) * cols, cols, 1).astype(jnp.float32)
            added = projected.astype(jnp.float32)
            out_square = lax.psum(jnp.sum(added * added, -1, keepdims=True), ("x", "c"))
            scale = lax.rsqrt(out_square / model + EPSILON)
            return (own + added * scale * post_gain[layer]).astype(jnp.bfloat16)


def solution(mesh):
    n_sp, n_tp = mesh.shape["sp"], mesh.shape["tp"]
    cut = Mesh(mesh.devices.reshape(n_sp // 2, 2, n_tp // 2, 2), ("h", "l", "x", "c"))
    sp, tp = ("h", "l"), ("x", "c")
    placed = (
        P(sp, tp),
        P(),
        P(None, sp, tp),
        P(None, sp, tp),
        P(None, None, tp),
        P(None, tp),
        P(None, tp),
        P(None, tp, sp),
        P(None, tp),
    )
    return jax.shard_map(local, mesh=cut, in_specs=placed, out_specs=P(sp, tp), check_vma=False)
```

```python
import jax
import jax.numpy as jnp
from jax import lax
from jax.sharding import Mesh, PartitionSpec as P

EPSILON = 1e-06
LN_EPSILON = 1e-05


GROUP = ("l", "x", "c")


def swapped(block, axes):
    size = 2 ** len(axes)
    return lax.ppermute(block, axes, [(i, size - 1 - i) for i in range(size)])


def ordered(index, own, other, axis):
    return jnp.where(
        index == 0, jnp.concatenate([own, other], axis), jnp.concatenate([other, own], axis)
    )


def part(array, index, axis):
    size = array.shape[axis] // 2
    return lax.dynamic_slice_in_dim(array, index * size, size, axis)


def paired(array, cut_axis, join_axis):
    l = lax.axis_index("l")
    other = swapped(part(array, 1 - l, cut_axis), ("l",))
    return ordered(l, part(array, l, cut_axis), other, join_axis)


def all_rows(block):
    l, x, c = (lax.axis_index(a) for a in GROUP)
    from_x = swapped(block, ("x",))
    from_l = swapped(block, ("l",))
    from_lx = swapped(block, ("l", "x"))
    mine = [block, from_x, from_l, from_lx]
    theirs = [swapped(b, ("c",)) for b in mine]
    cells = []
    for m, t in zip(mine, theirs):
        cells.append((jnp.where(c == 0, m, t), jnp.where(c == 0, t, m)))
    (a0, a1), (b0, b1), (p0, p1), (q0, q1) = cells
    near = jnp.where(x == 0, jnp.concatenate([a0, a1, b0, b1], 1), jnp.concatenate([b0, b1, a0, a1], 1))
    far = jnp.where(x == 0, jnp.concatenate([p0, p1, q0, q1], 1), jnp.concatenate([q0, q1, p0, p1], 1))
    return ordered(l, near, far, 0)


def group_sum(stats):
    stats = stats + swapped(stats, ("c",))
    return (stats + swapped(stats, ("x",))) + (swapped(stats, ("l",)) + swapped(stats, ("l", "x")))


def all_gains(gain):
    x, c = lax.axis_index("x"), lax.axis_index("c")
    near = ordered(c, gain, swapped(gain, ("c",)), 0)
    far = ordered(c, swapped(gain, ("x",)), swapped(gain, ("x", "c")), 0)
    return ordered(x, near, far, 0)


def scattered_sum(activated, out_mat):
    l, x, c = (lax.axis_index(a) for a in GROUP)
    cols = out_mat.shape[1] // 4
    rows = activated.shape[0] // 2

    def terms(x_at, c_at):
        mat = lax.dynamic_slice_in_dim(out_mat, (x_at * 2 + c_at) * cols, cols, 1)
        return jnp.dot(activated, mat, preferred_element_type=jnp.float32).astype(jnp.bfloat16)

    to_far, to_near = terms(1 - x, 1 - c), terms(x, 1 - c)
    far = terms(1 - x, c).astype(jnp.float32) + swapped(to_far, ("c",)).astype(jnp.float32)
    far = far.astype(jnp.bfloat16)
    near = terms(x, c).astype(jnp.float32) + swapped(to_near, ("c",)).astype(jnp.float32)
    near = near.astype(jnp.bfloat16)
    from_lx = swapped(part(far, 1 - l, 0), ("l", "x"))
    from_x = swapped(part(far, l, 0), ("x",))
    from_l = swapped(part(near, 1 - l, 0), ("l",))
    own = part(near, l, 0)
    total = own.astype(jnp.float32) + from_x.astype(jnp.float32)
    total = total + from_l.astype(jnp.float32) + from_lx.astype(jnp.float32)
    return total.astype(jnp.bfloat16)


def local(tokens, pre_gain, w_value, w_gate, taps, norm_gain, norm_shift, w_out, post_gain):
    l, x, c = (lax.axis_index(a) for a in GROUP)
    layers, width = taps.shape[:2]
    model = pre_gain.shape[1]
    n_h = lax.axis_size("h")
    pairs = []
    for layer in range(layers):
        own, other = (
            jnp.concatenate([part(w_value[layer], at, 1), part(w_gate[layer], at, 1)], 1)
            for at in (l, 1 - l)
        )
        pairs += [ordered(l, own, swapped(other, ("l",)), 0), paired(w_out[layer], 0, 1)]
    full_post = [all_gains(post_gain[layer]) for layer in range(layers - 1)]
    whole, full_post, pairs[1:] = lax.optimization_barrier(
        (all_rows(tokens), full_post, pairs[1:])
    )
    in_mats = [lax.all_gather(p, "h", axis=0, tiled=True) for p in pairs[::2]]
    out_mats = [lax.all_gather(p, "h", axis=1, tiled=True) for p in pairs[1::2]]
    rows = whole.shape[0]
    for layer in range(layers):
        whole_f = whole.astype(jnp.float32)
        normed = (
            whole_f
            * lax.rsqrt(jnp.mean(whole_f * whole_f, -1, keepdims=True) + EPSILON)
            * pre_gain[layer]
        ).astype(jnp.bfloat16)
        proj = jnp.dot(normed, in_mats[layer], preferred_element_type=jnp.float32)
        value_proj, gate_proj = jnp.split(proj, 2, 1)
        glu_act = (value_proj * jax.nn.sigmoid(gate_proj)).astype(jnp.bfloat16)
        fringe = lax.ppermute(
            glu_act[rows - (width - 1) :], "h", [(i, i + 1) for i in range(n_h - 1)]
        )
        padded = jnp.concatenate([fringe, glu_act], 0).astype(jnp.float32)
        tap = part(taps[layer], l, 1)
        conv_out = jnp.zeros(glu_act.shape, jnp.float32)
        for offset in range(width):
            conv_out = conv_out + tap[offset] * padded[offset : offset + rows]
        stats = group_sum(jnp.stack([jnp.sum(conv_out, -1), jnp.sum(conv_out * conv_out, -1)]))
        row_sum, row_square = stats[0][:, None], stats[1][:, None]
        center = row_sum / model
        spread = jnp.maximum(row_square / model - center * center, 0.0)
        activated = jax.nn.silu(
            (conv_out - center) * lax.rsqrt(spread + LN_EPSILON) * part(norm_gain[layer], l, 0)
            + part(norm_shift[layer], l, 0)
        ).astype(jnp.bfloat16)
        projected = scattered_sum(activated, out_mats[layer])
        if layer < layers - 1:
            added = all_rows(projected).astype(jnp.float32)
            scale = lax.rsqrt(jnp.mean(added * added, -1, keepdims=True) + EPSILON)
            whole = (whole_f + added * scale * full_post[layer]).astype(jnp.bfloat16)
        else:
            own = part(whole, l, 0)
            cols = tokens.shape[1]
            own = lax.dynamic_slice_in_dim(own, (x * 2 + c) * cols, cols, 1).astype(jnp.float32)
            added = projected.astype(jnp.float32)
            out_square = lax.psum(jnp.sum(added * added, -1, keepdims=True), ("x", "c"))
            scale = lax.rsqrt(out_square / model + EPSILON)
            return (own + added * scale * post_gain[layer]).astype(jnp.bfloat16)


def solution(mesh):
    n_sp, n_tp = mesh.shape["sp"], mesh.shape["tp"]
    cut = Mesh(mesh.devices.reshape(n_sp // 2, 2, n_tp // 2, 2), ("h", "l", "x", "c"))
    sp, tp = ("h", "l"), ("x", "c")
    placed = (
        P(sp, tp),
        P(),
        P(None, sp, tp),
        P(None, sp, tp),
        P(None, None, tp),
        P(None, tp),
        P(None, tp),
        P(None, tp, sp),
        P(None, tp),
    )
    return jax.shard_map(local, mesh=cut, in_specs=placed, out_specs=P(sp, tp), check_vma=False)
```
